32 devices in a mesh: fs: 8 (over z, x), tp: 4 (over y, core).
Axes of the slice: x: 2, y: 2, z: 4, core: 2. Of those that a mesh axis runs over, the one named last changes fastest.
Arguments:
- tokens: bfloat16 [8192, 2048], P('fs', 'tp'), may hold values from -6 to 6
- grad_out: bfloat16 [8192, 2048], P('fs', 'tp'), may hold values from -6 to 6
- norm_gain: float32 [2048], replicated, may hold values from 0.1 to 1.9
- gate_weight: bfloat16 [3072, 2048], P('tp', 'fs'), may hold values from -0.125 to 0.125
- up_weight: bfloat16 [3072, 2048], P('tp', 'fs'), may hold values from -0.125 to 0.125
- down_weight: bfloat16 [3072, 2048], P('tp', 'fs'), may hold values from -0.109375 to 0.109375
Outputs:
- grad_input: bfloat16 [8192, 2048], P('fs', 'tp')
- grad_gate: float32 [3072, 2048], P('tp', 'fs')
- grad_up: float32 [3072, 2048], P('tp', 'fs')
- grad_down: float32 [3072, 2048], P('tp', 'fs')
- row_squares: float32 [3, 3072], P(None, 'tp')
The draws below stay inside these ranges and needn't reach their ends.
All inputs are finite; a program needn't handle non-finite values.
Results may differ from the reference program's by a relative error of at most 0.015.
Values may be sent and summed in bfloat16 or wider, within the bound.
A program may use at most 64 MiB of HBM per device.

```python
import jax
import jax.numpy as jnp
from jax import lax

D = 2048
FF = 3072
TOKENS = 8192
N_TP = 4


def with_spikes(drawn, rng, source, target, blocks, factor):
    owner, partner = [(jnp.arange(drawn.shape[dim]) // (drawn.shape[dim] // blocks)).reshape([-1 if axis == dim else 1 for axis in range(drawn.ndim)]) for dim in (source, target)]
    chosen = jax.random.permutation(rng, blocks)[partner]
    strong = (owner == chosen) | (owner == (partner + blocks // 2) % blocks)
    return jnp.where(strong, factor * drawn, drawn)


def levels(own_key, dims, split, least, top_value):
    level, own = 1.0, jax.random.fold_in(own_key, 6)
    for position, shards_of in split:
        heights = jnp.exp(jax.random.uniform(jax.random.fold_in(own, position), (shards_of,), jnp.float32, least / len(split), top_value / len(split)))
        level = level * jnp.repeat(heights, dims[position] // shards_of).reshape([-1 if axis == position else 1 for axis in range(len(dims))])
    return level


def noise(stream_key, dims, scale, reach, pieces=(), dtype=jnp.bfloat16):
    loudness = levels(stream_key, dims, pieces, -0.22, 0.18) if pieces else 1.0
    entries = jax.random.normal(stream_key, dims, jnp.float32) * scale * loudness
    return jnp.minimum(jnp.maximum(entries, -reach), reach).astype(dtype)


def bell_draw_with(stream_key, extent, spread, bound, split, heavy, dtype=jnp.bfloat16):
    entries = spread * jax.random.normal(stream_key, extent, jnp.float32)
    if split:
        entries = entries * levels(stream_key, extent, split, -0.22, 0.18)
    return jnp.clip(with_spikes(entries, jax.random.fold_in(stream_key, 3), *heavy), -bound, bound).astype(dtype)


def setup_inputs(seed: int = 0) -> dict:
    key_list = jax.random.split(jax.random.key(seed), 7)
    tokens = noise(key_list[0], (TOKENS, D), 1.0, 6.0, ((0, 8), (1, 4)))
    grad_out = bell_draw_with(key_list[1], (TOKENS, D), 1.0, 6.0, ((0, 8), (1, 4)), (0, 1, 8, 2.0))
    norm_gain = jnp.clip(1.0 + 0.18 * jax.random.normal(key_list[2], (D,), jnp.float32), 0.1, 1.9)
    gate_weight = noise(key_list[3], (FF, D), D ** -0.5, 0.125, ((0, 4), (1, 8)))
    up_weight = noise(key_list[4], (FF, D), D ** -0.5, 0.125, ((0, 4), (1, 8)))
    down_weight = noise(key_list[5], (FF, D), FF ** -0.5, 0.109375, ((0, 4), (1, 8)))
    return {"tokens": tokens, "grad_out": grad_out, "norm_gain": norm_gain, "gate_weight": gate_weight, "up_weight": up_weight, "down_weight": down_weight}


def rms_back(grad_rows, unit_rows, inv_rms, gain_rows):
    scaled = gain_rows * grad_rows
    inner = lax.optimization_barrier(jnp.mean(scaled * unit_rows, axis=-1, keepdims=True))
    return inv_rms * (scaled - unit_rows * inner)

def reference(tokens, grad_out, norm_gain, gate_weight, up_weight, down_weight):
    floated = tokens.astype(jnp.float32)
    inv_rms = lax.rsqrt(lax.optimization_barrier(jnp.mean(floated * floated, axis=-1, keepdims=True)) + 1e-06)
    unit_rows = floated * inv_rms
    gain_rows = norm_gain.astype(jnp.float32)[None, :]
    normed = (unit_rows * gain_rows).astype(jnp.bfloat16)
    gate_pre = jnp.dot(normed, gate_weight.T, preferred_element_type=jnp.float32)
    up_pre = jnp.dot(normed, up_weight.T, preferred_element_type=jnp.float32)
    sigma = jax.nn.sigmoid(gate_pre)
    active = gate_pre * sigma
    hidden = (active * up_pre).astype(jnp.bfloat16)
    grad_hidden = 0.5 * jnp.dot(grad_out, down_weight.T, preferred_element_type=jnp.float32)
    gate_grad_pre = (grad_hidden * up_pre * sigma * (1.0 + gate_pre * (1.0 - sigma))).astype(jnp.bfloat16)
    up_grad_pre = (grad_hidden * active).astype(jnp.bfloat16)
    factor = TOKENS ** (-0.5)
    grad_down = 0.5 * factor * jnp.dot(hidden.T, grad_out, preferred_element_type=jnp.float32)
    grad_gate = factor * jnp.dot(gate_grad_pre.T, normed, preferred_element_type=jnp.float32)
    grad_up = factor * jnp.dot(up_grad_pre.T, normed, preferred_element_type=jnp.float32)
    width = FF // N_TP
    total = jnp.zeros(tokens.shape, jnp.float32)
    for block in range(N_TP):
        lower = block * width
        upper = lower + width
        grad_rows = jnp.dot(gate_grad_pre[:, lower:upper], gate_weight[lower:upper], preferred_element_type=jnp.float32)
        grad_rows = grad_rows + jnp.dot(up_grad_pre[:, lower:upper], up_weight[lower:upper], preferred_element_type=jnp.float32)
        partial_k = rms_back(grad_rows, unit_rows, inv_rms, gain_rows).astype(jnp.bfloat16)
        total = total + partial_k.astype(jnp.float32)
    grad_input = (grad_out.astype(jnp.float32) + total).astype(jnp.bfloat16)
    row_squares = jnp.stack([lax.optimization_barrier(jnp.sum(grad_gate * grad_gate, axis=1)), lax.optimization_barrier(jnp.sum(grad_up * grad_up, axis=1)), lax.optimization_barrier(jnp.sum(grad_down * grad_down, axis=1))]) / D
    return (grad_input, grad_gate, grad_up, grad_down, row_squares)
```

```python
import functools
import math

import jax
import jax.numpy as jnp
from jax import lax
from jax.experimental import pallas as pl
from jax.experimental.pallas import tpu as pltpu
from jax.sharding import PartitionSpec as P

MESH = pl.DeviceIdType.MESH
ANY = pl.BlockSpec(memory_space=pl.ANY)
VMEM = pl.BlockSpec(memory_space=pltpu.VMEM)


def contract(left, right, left_dim, right_dim):
    return lax.dot_general(
        left, right, (((left_dim,), (right_dim,)), ((), ())), preferred_element_type=jnp.float32
    )


def rms_back(grad_rows, unit_rows, inv_rms, gain_rows):
    scaled = gain_rows * grad_rows
    inner = jnp.mean(scaled * unit_rows, axis=-1, keepdims=True)
    return inv_rms * (scaled - unit_rows * inner)


def axes_of(n_fs, n_tp):
    nx = max(1, math.isqrt(max(1, n_fs // 2)))
    while n_fs % nx:
        nx -= 1
    nc = 2 if n_tp % 2 == 0 else 1
    return n_fs // nx, nx, n_tp // nc, nc


def greet(targets):
    barrier = pltpu.get_barrier_semaphore()
    for target in targets:
        pl.semaphore_signal(barrier, inc=1, device_id=target, device_id_type=MESH)
    pl.semaphore_wait(barrier, len(targets))


def remote(src, dst, send_sem, recv_sem, target):
    return pltpu.make_async_remote_copy(
        src_ref=src, dst_ref=dst, send_sem=send_sem, recv_sem=recv_sem,
        device_id=target, device_id_type=MESH,
    )


def block_of(ref, index, width):
    if len(ref.shape) == 3:
        return ref.at[index]
    return ref.at[:, pl.ds(pl.multiple_of(index * width, 128), width)]


def gather_kernel(dims, *refs):
    nz, nx, ny, nc = dims
    small, full, held = refs[:5], refs[5:10], refs[10:15]
    out_sem, in_sem, zs, zr, xs, xr, ys, yr, cs, cr = refs[15:]
    fs, tp = lax.axis_index("fs"), lax.axis_index("tp")
    z, x, y, c = fs // nx, fs % nx, tp // nc, tp % nc

    def z_dev(r):
        return {"fs": lax.rem(z + r, nz) * nx + x}

    def x_dev(q):
        return {"fs": z * nx + lax.rem(x + q, nx)}

    def y_dev(r):
        return {"tp": lax.rem(y + r, ny) * nc + c}

    def c_dev(q):
        return {"tp": y * nc + lax.rem(c + q, nc)}

    greet(
        [z_dev(r) for r in range(1, nz)] + [x_dev(q) for q in range(1, nx)]
        + [y_dev(r) for r in range(1, ny)] + [c_dev(q) for q in range(1, nc)]
    )
    width = [ref.shape[1] for ref in small]
    sends = []

    def go(copy):
        copy.start()
        sends.append(copy)

    acts, mats = (0, 1), (2, 3, 4)
    for a in acts:
        for r in range(1, ny):
            go(remote(small[a], block_of(full[a], tp, width[a]), ys.at[a, r], yr.at[a, r], y_dev(r)))
    z_order = [r for r in range(2, nz)] + [1] if nz > 1 else []
    for m in mats:
        for r in z_order:
            go(remote(small[m], block_of(full[m], fs, width[m]), zs.at[m - 2, r], zr.at[m - 2, r], z_dev(r)))
        for q in range(1, nx):
            go(remote(small[m], block_of(full[m], fs, width[m]), xs.at[m - 2, 0, q], xr.at[m - 2, 0, q], x_dev(q)))
    for a in acts:
        for q in range(1, nc):
            go(remote(small[a], block_of(full[a], tp, width[a]), cs.at[a, 0, q], cr.at[a, 0, q], c_dev(q)))
    loads = [pltpu.make_async_copy(small[i], held[i], in_sem.at[i]) for i in range(5)]
    for load in loads:
        load.start()
    stores = []
    for i in range(5):
        loads[i].wait()
        index = tp if i < 2 else fs
        stores.append(pltpu.make_async_copy(held[i], block_of(full[i], index, width[i]), out_sem.at[i]))
        stores[i].start()

    def from_y(a, r):
        origin = lax.rem(y + ny - r, ny) * nc + c
        block = block_of(full[a], origin, width[a])
        remote(block, block, ys.at[a, r], yr.at[a, r], y_dev(r)).wait_recv()
        for q in range(1, nc):
            go(remote(block, block, cs.at[a, r, q], cr.at[a, r, q], c_dev(q)))

    def from_z(m, r):
        origin = lax.rem(z + nz - r, nz) * nx + x
        block = block_of(full[m], origin, width[m])
        remote(block, block, zs.at[m - 2, r], zr.at[m - 2, r], z_dev(r)).wait_recv()
        for q in range(1, nx):
            go(remote(block, block, xs.at[m - 2, r, q], xr.at[m - 2, r, q], x_dev(q)))

    late = [(a, r) for a in acts for r in range(1, ny)]
    for m in mats:
        for r in z_order:
            from_z(m, r)
        if late:
            from_y(*late.pop(0))
    for a, r in late:
        from_y(a, r)
    for m in mats:
        for r in range(nz):
            for q in range(1, nx):
                origin = lax.rem(z + nz - r, nz) * nx + lax.rem(x + nx - q, nx)
                block = block_of(full[m], origin, width[m])
                remote(block, block, xs.at[m - 2, r, q], xr.at[m - 2, r, q], x_dev(q)).wait_recv()
    for a in acts:
        for r in range(ny):
            for q in range(1, nc):
                origin = lax.rem(y + ny - r, ny) * nc + lax.rem(c + nc - q, nc)
                block = block_of(full[a], origin, width[a])
                remote(block, block, cs.at[a, r, q], cr.at[a, r, q], c_dev(q)).wait_recv()
    for store in stores:
        store.wait()
    for copy in sends:
        copy.wait_send()


def gather_all(dims, arrays):
    nz, nx, ny, nc = dims
    shapes = []
    for i, a in enumerate(arrays):
        n = ny * nc if i < 2 else nz * nx
        rows, cols = a.shape
        shape = (rows, n * cols) if cols % 128 == 0 else (n, rows, cols)
        shapes.append(jax.ShapeDtypeStruct(shape, a.dtype))
    dma = pltpu.SemaphoreType.DMA
    full = pl.pallas_call(
        functools.partial(gather_kernel, dims),
        out_shape=shapes,
        in_specs=[ANY] * 5,
        out_specs=[ANY] * 5,
        scratch_shapes=[pltpu.VMEM(a.shape, a.dtype) for a in arrays]
        + [
            dma((5,)), dma((5,)), dma((3, nz)), dma((3, nz)), dma((3, nz, nx)), dma((3, nz, nx)),
            dma((2, ny)), dma((2, ny)), dma((2, ny, nc)), dma((2, ny, nc)),
        ],
        compiler_params=pltpu.CompilerParams(collective_id=0, has_side_effects=True),
        name="gather",
    )(*arrays)
    return [
        a if a.ndim == 2 else jnp.swapaxes(a, 0, 1).reshape(a.shape[1], -1) for a in full
    ]


def reduce_kernel(dims, width_total, *refs):
    nz, nx, ny, nc = dims
    terms, part, grad = refs[:3], refs[3], refs[4]
    outs, out_x, out_sq = refs[5:8], refs[8], refs[9]
    (own, x_in, z_out, z_in, p_own, c_in, y_out, y_in, sq_out, sq_in,
     own_sem, p_sem, xs, xr, zs, zr, cs, cr, ys, yr, qs, qr) = refs[10:]
    n_fs = nz * nx
    fs, tp = lax.axis_index("fs"), lax.axis_index("tp")
    z, x, y, c = fs // nx, fs % nx, tp // nc, tp % nc
    width, cols = outs[0].shape[1], out_x.shape[1]
    f32, bf16 = jnp.float32, jnp.bfloat16

    def z_index(r):
        return lax.rem(z + r, nz) * nx + x

    def fs_dev(k):
        return {"fs": lax.rem(fs + k, n_fs)}

    def x_dev(q):
        return {"fs": z * nx + lax.rem(x + q, nx)}

    def y_dev(r):
        return {"tp": lax.rem(y + r, ny) * nc + c}

    def c_dev(q):
        return {"tp": y * nc + lax.rem(c + q, nc)}

    greet(
        [fs_dev(k) for k in range(1, n_fs)]
        + [y_dev(r) for r in range(1, ny)] + [c_dev(q) for q in range(1, nc)]
    )
    sends = []

    def go(copy):
        copy.start()
        sends.append(copy)

    z_order = ([r for r in range(2, nz)] + [1] if nz > 1 else []) + [0]
    y_order = [r for r in range(1, ny)] + [0]
    for r in y_order:
        for q in range(1, nc):
            index = lax.rem(y + r, ny) * nc + lax.rem(c + q, nc)
            go(remote(block_of(part, index, cols), c_in.at[r, q - 1], cs.at[r, q], cr.at[r, q], c_dev(q)))
    for r in z_order:
        for w in range(3):
            for q in range(1, nx):
                index = lax.rem(z + r, nz) * nx + lax.rem(x + q, nx)
                go(remote(block_of(terms[w], index, width), x_in.at[w, r, q - 1], xs.at[w, r, q], xr.at[w, r, q], x_dev(q)))
    p_loads = {}
    for r in y_order:
        index = lax.rem(y + r, ny) * nc + c
        p_loads[r] = pltpu.make_async_copy(block_of(part, index, cols), p_own.at[r], p_sem.at[r])
        p_loads[r].start()
    loads = {}
    for r in z_order:
        for w in range(3):
            loads[w, r] = pltpu.make_async_copy(block_of(terms[w], z_index(r), width), own.at[w, r], own_sem.at[w, r])
            loads[w, r].start()

    def pair_wait(r):
        p_loads[r].wait()
        for q in range(1, nc):
            remote(p_own.at[r], c_in.at[r, q - 1], cs.at[r, q], cr.at[r, q], c_dev(q)).wait_recv()

    def wide_wait(w, r):
        loads[w, r].wait()
        for q in range(1, nx):
            remote(own.at[w, r], x_in.at[w, r, q - 1], xs.at[w, r, q], xr.at[w, r, q], x_dev(q)).wait_recv()

    def tiles(rows, body):
        step = math.gcd(rows, 128)

        def run(i, carry):
            body(pl.ds(pl.multiple_of(i * step, step), step))
            return carry

        lax.fori_loop(0, rows // step, run, 0)

    n_rows, n_hid = out_x.shape[0], outs[0].shape[0]
    for r in range(1, ny):
        pair_wait(r)

        def add_pair(rows):
            acc = p_own[r, rows, :].astype(f32)
            for q in range(1, nc):
                acc = acc + c_in[r, q - 1, rows, :].astype(f32)
            y_out[r, rows, :] = acc.astype(bf16)

        tiles(n_rows, add_pair)
        go(remote(y_out.at[r], y_in.at[r], ys.at[r], yr.at[r], y_dev(r)))
    for r in z_order[:-1]:
        for w in range(3):
            wide_wait(w, r)

            def add_wide(rows):
                acc = own[w, r, rows, :].astype(f32)
                for q in range(1, nx):
                    acc = acc + x_in[w, r, q - 1, rows, :].astype(f32)
                z_out[w, r, rows, :] = acc.astype(bf16)

            tiles(n_hid, add_wide)
            go(remote(z_out.at[w, r], z_in.at[w, r], zs.at[w, r], zr.at[w, r], {"fs": z_index(r)}))
    pair_wait(0)
    for r in range(1, ny):
        remote(y_out.at[r], y_in.at[r], ys.at[r], yr.at[r], y_dev(r)).wait_recv()

    def finish_rows(rows):
        acc = grad[rows, :].astype(f32) + p_own[0, rows, :].astype(f32)
        for q in range(1, nc):
            acc = acc + c_in[0, q - 1, rows, :].astype(f32)
        for r in range(1, ny):
            acc = acc + y_in[r, rows, :].astype(f32)
        out_x[rows, :] = acc.astype(bf16)

    tiles(n_rows, finish_rows)
    ones = jnp.ones((8, width), f32)
    for w in range(3):
        wide_wait(w, 0)
        for r in z_order[:-1]:
            remote(z_out.at[w, r], z_in.at[w, r], zs.at[w, r], zr.at[w, r], {"fs": z_index(r)}).wait_recv()

        def finish_term(rows):
            acc = own[w, 0, rows, :].astype(f32)
            for q in range(1, nx):
                acc = acc + x_in[w, 0, q - 1, rows, :].astype(f32)
            for r in z_order[:-1]:
                acc = acc + z_in[w, r, rows, :].astype(f32)
            outs[w][rows, :] = acc
            squares = lax.dot_general(
                ones, acc * acc, (((1,), (1,)), ((), ())),
                precision=lax.Precision.HIGHEST, preferred_element_type=f32,
            )
            sq_out[pl.ds(w, 1), rows] = squares[:1]

        tiles(n_hid, finish_term)
    for k in range(1, n_fs):
        go(remote(sq_out, sq_in.at[k], qs.at[k], qr.at[k], fs_dev(k)))
    total = sq_out[...]
    for k in range(1, n_fs):
        remote(sq_out, sq_in.at[k], qs.at[k], qr.at[k], fs_dev(k)).wait_recv()
        total = total + sq_in[k]
    out_sq[...] = total / width_total
    for copy in sends:
        copy.wait_send()


def reduce_all(dims, terms, part, grad_out, width):
    nz, nx, ny, nc = dims
    n_fs = nz * nx
    hid = terms[0].shape[0]
    rows, cols = grad_out.shape
    if width % 128:
        terms = [jnp.swapaxes(t.reshape(hid, n_fs, width), 0, 1) for t in terms]
    dma, bf16, f32 = pltpu.SemaphoreType.DMA, jnp.bfloat16, jnp.float32
    return pl.pallas_call(
        functools.partial(reduce_kernel, dims, n_fs * width),
        out_shape=[jax.ShapeDtypeStruct((hid, width), f32)] * 3
        + [jax.ShapeDtypeStruct((rows, cols), bf16), jax.ShapeDtypeStruct((3, hid), f32)],
        in_specs=[ANY] * 4 + [VMEM],
        out_specs=[VMEM] * 5,
        scratch_shapes=[
            pltpu.VMEM((3, nz, hid, width), bf16),
            pltpu.VMEM((3, nz, max(1, nx - 1), hid, width), bf16),
            pltpu.VMEM((3, nz, hid, width), bf16),
            pltpu.VMEM((3, nz, hid, width), bf16),
            pltpu.VMEM((ny, rows, cols), bf16),
            pltpu.VMEM((ny, max(1, nc - 1), rows, cols), bf16),
            pltpu.VMEM((ny, rows, cols), bf16),
            pltpu.VMEM((ny, rows, cols), bf16),
            pltpu.VMEM((3, hid), f32),
            pltpu.VMEM((n_fs, 3, hid), f32),
            dma((3, nz)), dma((ny,)),
            dma((3, nz, nx)), dma((3, nz, nx)), dma((3, nz)), dma((3, nz)),
            dma((ny, nc)), dma((ny, nc)), dma((ny,)), dma((ny,)),
            dma((n_fs,)), dma((n_fs,)),
        ],
        compiler_params=pltpu.CompilerParams(
            collective_id=1, has_side_effects=True, vmem_limit_bytes=60 * 2**20
        ),
        name="reduce",
    )(*terms, part, grad_out)


def on_device(dims, tokens, grad_out, norm_gain, gate_weight, up_weight, down_weight):
    full_tokens, full_grad, gate_full, up_full, down_full = gather_all(
        dims, (tokens, grad_out, gate_weight, up_weight, down_weight)
    )
    floated = full_tokens.astype(jnp.float32)
    inv_rms = lax.rsqrt(jnp.mean(floated * floated, axis=-1, keepdims=True) + 1e-06)
    unit_rows = floated * inv_rms
    gain_rows = norm_gain[None, :]
    normed = (unit_rows * gain_rows).astype(jnp.bfloat16)
    grad_hidden = 0.5 * contract(full_grad, down_full, 1, 1)
    factor = (full_tokens.shape[0] * lax.axis_size("fs")) ** (-0.5)
    gate_pre = contract(normed, gate_full, 1, 1)
    up_pre = contract(normed, up_full, 1, 1)
    sigma = jax.nn.sigmoid(gate_pre)
    active = gate_pre * sigma
    hidden = (active * up_pre).astype(jnp.bfloat16)
    term_down = 0.5 * factor * contract(hidden, full_grad, 0, 0)
    gate_grad_pre = (grad_hidden * up_pre * sigma * (1.0 + gate_pre * (1.0 - sigma))).astype(
        jnp.bfloat16
    )
    term_gate = factor * contract(gate_grad_pre, normed, 0, 0)
    up_grad_pre = (grad_hidden * active).astype(jnp.bfloat16)
    term_up = factor * contract(up_grad_pre, normed, 0, 0)
    grad_rows = jnp.dot(gate_grad_pre, gate_full, preferred_element_type=jnp.float32)
    grad_rows = grad_rows + jnp.dot(up_grad_pre, up_full, preferred_element_type=jnp.float32)
    partial_value = rms_back(grad_rows, unit_rows, inv_rms, gain_rows).astype(jnp.bfloat16)
    terms = [t.astype(jnp.bfloat16) for t in (term_gate, term_up, term_down)]
    grad_gate, grad_up, grad_down, grad_input, row_squares = reduce_all(
        dims, terms, partial_value, grad_out, gate_weight.shape[1]
    )
    return (grad_input, grad_gate, grad_up, grad_down, row_squares)


def solution(mesh):
    in_specs = (P("fs", "tp"), P("fs", "tp"), P(), P("tp", "fs"), P("tp", "fs"), P("tp", "fs"))
    out_specs = (P("fs", "tp"), P("tp", "fs"), P("tp", "fs"), P("tp", "fs"), P(None, "tp"))
    dims = axes_of(mesh.shape["fs"], mesh.shape["tp"])
    return jax.shard_map(
        functools.partial(on_device, dims), mesh=mesh, in_specs=in_specs, out_specs=out_specs,
        check_vma=False,
    )
```

```python
import functools
import math

import jax
import jax.numpy as jnp
from jax import lax
from jax.experimental import pallas as pl
from jax.experimental.pallas import tpu as pltpu
from jax.sharding import PartitionSpec as P

MESH = pl.DeviceIdType.MESH
ANY = pl.BlockSpec(memory_space=pl.ANY)
VMEM = pl.BlockSpec(memory_space=pltpu.VMEM)


def contract(left, right, left_dim, right_dim):
    return lax.dot_general(
        left, right, (((left_dim,), (right_dim,)), ((), ())), preferred_element_type=jnp.float32
    )


def rms_back(grad_rows, unit_rows, inv_rms, gain_rows):
    scaled = gain_rows * grad_rows
    inner = jnp.mean(scaled * unit_rows, axis=-1, keepdims=True)
    return inv_rms * (scaled - unit_rows * inner)


def axes_of(n_fs, n_tp):
    nx = max(1, math.isqrt(max(1, n_fs // 2)))
    while n_fs % nx:
        nx -= 1
    nc = 2 if n_tp % 2 == 0 else 1
    return n_fs // nx, nx, n_tp // nc, nc


def greet(targets):
    barrier = pltpu.get_barrier_semaphore()
    for target in targets:
        pl.semaphore_signal(barrier, inc=1, device_id=target, device_id_type=MESH)
    pl.semaphore_wait(barrier, len(targets))


def remote(src, dst, send_sem, recv_sem, target):
    return pltpu.make_async_remote_copy(
        src_ref=src, dst_ref=dst, send_sem=send_sem, recv_sem=recv_sem,
        device_id=target, device_id_type=MESH,
    )


def block_of(ref, index, width):
    if len(ref.shape) == 3:
        return ref.at[index]
    return ref.at[:, pl.ds(pl.multiple_of(index * width, 128), width)]


def gather_kernel(dims, *refs):
    nz, nx, ny, nc = dims
    small, full, held = refs[:5], refs[5:10], refs[10:15]
    out_sem, in_sem, zs, zr, xs, xr, ys, yr, cs, cr = refs[15:]
    fs, tp = lax.axis_index("fs"), lax.axis_index("tp")
    z, x, y, c = fs // nx, fs % nx, tp // nc, tp % nc

    def z_dev(r):
        return {"fs": lax.rem(z + r, nz) * nx + x}

    def x_dev(q):
        return {"fs": z * nx + lax.rem(x + q, nx)}

    def y_dev(r):
        return {"tp": lax.rem(y + r, ny) * nc + c}

    def c_dev(q):
        return {"tp": y * nc + lax.rem(c + q, nc)}

    greet(
        [z_dev(r) for r in range(1, nz)] + [x_dev(q) for q in range(1, nx)]
        + [y_dev(r) for r in range(1, ny)] + [c_dev(q) for q in range(1, nc)]
    )
    width = [ref.shape[1] for ref in small]
    sends = []

    def go(copy):
        copy.start()
        sends.append(copy)

    acts, mats = (0, 1), (2, 3, 4)
    for a in acts:
        for r in range(1, ny):
            go(remote(small[a], block_of(full[a], tp, width[a]), ys.at[a, r], yr.at[a, r], y_dev(r)))
    def along(way, m, d):
        origin = lax.rem(z + nz - way * (d - 1), nz) * nx + x
        block = block_of(full[m], origin, width[m])
        lane = (1 - way) // 2
        return remote(
            small[m] if d == 1 else block, block, zs.at[lane, m - 2, d], zr.at[lane, m - 2, d],
            {"fs": lax.rem(z + nz + way, nz) * nx + x},
        )

    def has_next(way):
        return z + 1 < nz if way == 1 else z >= 1

    def has_back(way, d):
        return z >= d if way == 1 else z + d < nz

    for m in mats:
        for way in (1, -1):
            if nz > 1:
                pl.when(has_next(way))(along(way, m, 1).start)
        for q in range(1, nx):
            go(remote(small[m], block_of(full[m], fs, width[m]), xs.at[m - 2, 0, q], xr.at[m - 2, 0, q], x_dev(q)))
    for a in acts:
        for q in range(1, nc):
            go(remote(small[a], block_of(full[a], tp, width[a]), cs.at[a, 0, q], cr.at[a, 0, q], c_dev(q)))
    loads = [pltpu.make_async_copy(small[i], held[i], in_sem.at[i]) for i in range(5)]
    for load in loads:
        load.start()
    stores = []
    for i in range(5):
        loads[i].wait()
        index = tp if i < 2 else fs
        stores.append(pltpu.make_async_copy(held[i], block_of(full[i], index, width[i]), out_sem.at[i]))
        stores[i].start()

    def from_y(a, r):
        origin = lax.rem(y + ny - r, ny) * nc + c
        block = block_of(full[a], origin, width[a])
        remote(block, block, ys.at[a, r], yr.at[a, r], y_dev(r)).wait_recv()
        for q in range(1, nc):
            go(remote(block, block, cs.at[a, r, q], cr.at[a, r, q], c_dev(q)))

    def from_z(way, m, d):
        origin = lax.rem(z + nz - way * d, nz) * nx + x
        block = block_of(full[m], origin, width[m])
        lane = (1 - way) // 2
        r = d if way == 1 else nz - d
        target = {"fs": lax.rem(z + nz + way, nz) * nx + x}
        remote(block, block, zs.at[lane, m - 2, d], zr.at[lane, m - 2, d], target).wait_recv()
        if d + 1 < nz:
            pl.when(has_next(way))(along(way, m, d + 1).start)
        for q in range(1, nx):
            remote(block, block, xs.at[m - 2, r, q], xr.at[m - 2, r, q], x_dev(q)).start()

    late = [(a, r) for a in acts for r in range(1, ny)]
    for d in range(1, nz):
        for m in mats:
            for way in (1, -1):
                pl.when(has_back(way, d))(functools.partial(from_z, way, m, d))
            if late:
                from_y(*late.pop(0))
    for a, r in late:
        from_y(a, r)
    for m in mats:
        for r in range(nz):
            for q in range(1, nx):
                origin = lax.rem(z + nz - r, nz) * nx + lax.rem(x + nx - q, nx)
                block = block_of(full[m], origin, width[m])
                remote(block, block, xs.at[m - 2, r, q], xr.at[m - 2, r, q], x_dev(q)).wait_recv()
    for a in acts:
        for r in range(ny):
            for q in range(1, nc):
                origin = lax.rem(y + ny - r, ny) * nc + lax.rem(c + nc - q, nc)
                block = block_of(full[a], origin, width[a])
                remote(block, block, cs.at[a, r, q], cr.at[a, r, q], c_dev(q)).wait_recv()
    for store in stores:
        store.wait()
    for m in mats:
        for d in range(1, nz):
            for way in (1, -1):
                sent = has_next(way) if d == 1 else has_next(way) & has_back(way, d - 1)
                pl.when(sent)(along(way, m, d).wait_send)
            origin = lax.rem(z + nz - d, nz) * nx + x
            block = block_of(full[m], origin, width[m])
            for q in range(1, nx):
                remote(block, block, xs.at[m - 2, d, q], xr.at[m - 2, d, q], x_dev(q)).wait_send()
    for copy in sends:
        copy.wait_send()


def gather_all(dims, arrays):
    nz, nx, ny, nc = dims
    shapes = []
    for i, a in enumerate(arrays):
        n = ny * nc if i < 2 else nz * nx
        rows, cols = a.shape
        shape = (rows, n * cols) if cols % 128 == 0 else (n, rows, cols)
        shapes.append(jax.ShapeDtypeStruct(shape, a.dtype))
    dma = pltpu.SemaphoreType.DMA
    full = pl.pallas_call(
        functools.partial(gather_kernel, dims),
        out_shape=shapes,
        in_specs=[ANY] * 5,
        out_specs=[ANY] * 5,
        scratch_shapes=[pltpu.VMEM(a.shape, a.dtype) for a in arrays]
        + [
            dma((5,)), dma((5,)), dma((2, 3, nz)), dma((2, 3, nz)), dma((3, nz, nx)), dma((3, nz, nx)),
            dma((2, ny)), dma((2, ny)), dma((2, ny, nc)), dma((2, ny, nc)),
        ],
        compiler_params=pltpu.CompilerParams(collective_id=0, has_side_effects=True),
        name="gather",
    )(*arrays)
    return [
        a if a.ndim == 2 else jnp.swapaxes(a, 0, 1).reshape(a.shape[1], -1) for a in full
    ]


def reduce_kernel(dims, width_total, *refs):
    nz, nx, ny, nc = dims
    terms, part, grad = refs[:3], refs[3], refs[4]
    outs, out_x, out_sq = refs[5:8], refs[8], refs[9]
    (own, x_in, z_out, up_in, down_in, p_own, c_in, y_out, y_in, sq_out, sq_in,
     own_sem, p_sem, xs, xr, zs, zr, cs, cr, ys, yr, qs, qr) = refs[10:]
    n_fs = nz * nx
    fs, tp = lax.axis_index("fs"), lax.axis_index("tp")
    z, x, y, c = fs // nx, fs % nx, tp // nc, tp % nc
    width, cols = outs[0].shape[1], out_x.shape[1]
    f32, bf16 = jnp.float32, jnp.bfloat16

    def z_index(r):
        return lax.rem(z + r, nz) * nx + x

    def fs_dev(k):
        return {"fs": lax.rem(fs + k, n_fs)}

    def x_dev(q):
        return {"fs": z * nx + lax.rem(x + q, nx)}

    def y_dev(r):
        return {"tp": lax.rem(y + r, ny) * nc + c}

    def c_dev(q):
        return {"tp": y * nc + lax.rem(c + q, nc)}

    greet(
        [fs_dev(k) for k in range(1, n_fs)]
        + [y_dev(r) for r in range(1, ny)] + [c_dev(q) for q in range(1, nc)]
    )
    sends = []

    def go(copy):
        copy.start()
        sends.append(copy)

    z_in = {1: up_in, -1: down_in}

    def has_next(way, d=1):
        return z + d < nz if way == 1 else z >= d

    def slot(way, d):
        return d if way == 1 else nz - d

    y_order = [r for r in range(1, ny)] + [0]
    for r in y_order:
        for q in range(1, nc):
            index = lax.rem(y + r, ny) * nc + lax.rem(c + q, nc)
            go(remote(block_of(part, index, cols), c_in.at[r, q - 1], cs.at[r, q], cr.at[r, q], c_dev(q)))
    def widely(w, r, q):
        index = lax.rem(z + r, nz) * nx + lax.rem(x + q, nx)
        return remote(block_of(terms[w], index, width), x_in.at[w, r, q - 1], xs.at[w, r, q], xr.at[w, r, q], x_dev(q))

    def widely_all(r):
        for w in range(3):
            for q in range(1, nx):
                widely(w, r, q).start()

    for d in range(nz - 1, 0, -1):
        for way in (1, -1):
            pl.when(has_next(way, d))(functools.partial(widely_all, slot(way, d)))
    widely_all(0)
    p_loads = {}
    for r in y_order:
        index = lax.rem(y + r, ny) * nc + c
        p_loads[r] = pltpu.make_async_copy(block_of(part, index, cols), p_own.at[r], p_sem.at[r])
        p_loads[r].start()
    loads = {}
    for r in range(nz):
        for w in range(3):
            loads[w, r] = pltpu.make_async_copy(block_of(terms[w], z_index(r), width), own.at[w, r], own_sem.at[w, r])
            loads[w, r].start()

    def pair_wait(r):
        p_loads[r].wait()
        for q in range(1, nc):
            remote(p_own.at[r], c_in.at[r, q - 1], cs.at[r, q], cr.at[r, q], c_dev(q)).wait_recv()

    def wide_wait(w, r):
        loads[w, r].wait()
        for q in range(1, nx):
            remote(own.at[w, r], x_in.at[w, r, q - 1], xs.at[w, r, q], xr.at[w, r, q], x_dev(q)).wait_recv()

    def tiles(rows, body):
        step = math.gcd(rows, 128)

        def run(i, carry):
            body(pl.ds(pl.multiple_of(i * step, step), step))
            return carry

        lax.fori_loop(0, rows // step, run, 0)

    n_rows, n_hid = out_x.shape[0], outs[0].shape[0]
    for r in range(1, ny):
        pair_wait(r)

        def add_pair(rows):
            acc = p_own[r, rows, :].astype(f32)
            for q in range(1, nc):
                acc = acc + c_in[r, q - 1, rows, :].astype(f32)
            y_out[r, rows, :] = acc.astype(bf16)

        tiles(n_rows, add_pair)
        go(remote(y_out.at[r], y_in.at[r], ys.at[r], yr.at[r], y_dev(r)))
    def along(way, w, d):
        r = slot(way, d)
        lane = (1 - way) // 2
        return remote(
            z_out.at[w, r], z_in[way].at[w, d - 1], zs.at[w, r], zr.at[lane, w, d - 1],
            {"fs": lax.rem(z + nz + way, nz) * nx + x},
        )

    def arrive(way, w, d):
        lane = (1 - way) // 2
        remote(
            z_out.at[w, 0], z_in[way].at[w, d], zs.at[w, 0], zr.at[lane, w, d],
            {"fs": lax.rem(z + nz + way, nz) * nx + x},
        ).wait_recv()

    def clear(way):
        def rows_clear(rows):
            for w in range(3):
                for d in range(nz):
                    z_in[way][w, d, rows, :] = jnp.zeros((rows.size, width), bf16)

        tiles(n_hid, rows_clear)

    pl.when(z == 0)(functools.partial(clear, 1))
    pl.when(z == nz - 1)(functools.partial(clear, -1))

    def pass_on(way, w, d):
        r = slot(way, d)
        wide_wait(w, r)
        if d < nz - 1:
            pl.when(has_next(-way))(functools.partial(arrive, way, w, d))

        def add_wide(rows):
            acc = own[w, r, rows, :].astype(f32)
            for q in range(1, nx):
                acc = acc + x_in[w, r, q - 1, rows, :].astype(f32)
            if d < nz - 1:
                acc = acc + z_in[way][w, d, rows, :].astype(f32)
            z_out[w, r, rows, :] = acc.astype(bf16)

        tiles(n_hid, add_wide)
        along(way, w, d).start()

    for d in range(nz - 1, 0, -1):
        for way in (1, -1):
            for w in range(3):
                pl.when(has_next(way, d))(functools.partial(pass_on, way, w, d))
    pair_wait(0)
    for r in range(1, ny):
        remote(y_out.at[r], y_in.at[r], ys.at[r], yr.at[r], y_dev(r)).wait_recv()

    def finish_rows(rows):
        acc = grad[rows, :].astype(f32) + p_own[0, rows, :].astype(f32)
        for q in range(1, nc):
            acc = acc + c_in[0, q - 1, rows, :].astype(f32)
        for r in range(1, ny):
            acc = acc + y_in[r, rows, :].astype(f32)
        out_x[rows, :] = acc.astype(bf16)

    tiles(n_rows, finish_rows)
    ones = jnp.ones((8, width), f32)
    for w in range(3):
        wide_wait(w, 0)
        for way in (1, -1):
            if nz > 1:
                pl.when(has_next(-way))(functools.partial(arrive, way, w, 0))

        def finish_term(rows):
            acc = own[w, 0, rows, :].astype(f32)
            for q in range(1, nx):
                acc = acc + x_in[w, 0, q - 1, rows, :].astype(f32)
            for way in (1, -1):
                acc = acc + z_in[way][w, 0, rows, :].astype(f32)
            outs[w][rows, :] = acc
            squares = lax.dot_general(
                ones, acc * acc, (((1,), (1,)), ((), ())),
                precision=lax.Precision.HIGHEST, preferred_element_type=f32,
            )
            sq_out[pl.ds(w, 1), rows] = squares[:1]

        tiles(n_hid, finish_term)
    for k in range(1, n_fs):
        go(remote(sq_out, sq_in.at[k], qs.at[k], qr.at[k], fs_dev(k)))
    total = sq_out[...]
    for k in range(1, n_fs):
        remote(sq_out, sq_in.at[k], qs.at[k], qr.at[k], fs_dev(k)).wait_recv()
        total = total + sq_in[k]
    out_sq[...] = total / width_total
    for w in range(3):
        for r in range(nz):
            for q in range(1, nx):
                widely(w, r, q).wait_send()
        for d in range(1, nz):
            for way in (1, -1):
                pl.when(has_next(way, d))(along(way, w, d).wait_send)
    for copy in sends:
        copy.wait_send()


def reduce_all(dims, terms, part, grad_out, width):
    nz, nx, ny, nc = dims
    n_fs = nz * nx
    hid = terms[0].shape[0]
    rows, cols = grad_out.shape
    if width % 128:
        terms = [jnp.swapaxes(t.reshape(hid, n_fs, width), 0, 1) for t in terms]
    dma, bf16, f32 = pltpu.SemaphoreType.DMA, jnp.bfloat16, jnp.float32
    return pl.pallas_call(
        functools.partial(reduce_kernel, dims, n_fs * width),
        out_shape=[jax.ShapeDtypeStruct((hid, width), f32)] * 3
        + [jax.ShapeDtypeStruct((rows, cols), bf16), jax.ShapeDtypeStruct((3, hid), f32)],
        in_specs=[ANY] * 4 + [VMEM],
        out_specs=[VMEM] * 5,
        scratch_shapes=[
            pltpu.VMEM((3, nz, hid, width), bf16),
            pltpu.VMEM((3, nz, max(1, nx - 1), hid, width), bf16),
            pltpu.VMEM((3, nz, hid, width), bf16),
            pltpu.VMEM((3, nz, hid, width), bf16),
            pltpu.VMEM((3, nz, hid, width), bf16),
            pltpu.VMEM((ny, rows, cols), bf16),
            pltpu.VMEM((ny, max(1, nc - 1), rows, cols), bf16),
            pltpu.VMEM((ny, rows, cols), bf16),
            pltpu.VMEM((ny, rows, cols), bf16),
            pltpu.VMEM((3, hid), f32),
            pltpu.VMEM((n_fs, 3, hid), f32),
            dma((3, nz)), dma((ny,)),
            dma((3, nz, nx)), dma((3, nz, nx)), dma((3, nz)), dma((2, 3, nz)),
            dma((ny, nc)), dma((ny, nc)), dma((ny,)), dma((ny,)),
            dma((n_fs,)), dma((n_fs,)),
        ],
        compiler_params=pltpu.CompilerParams(
            collective_id=1, has_side_effects=True, vmem_limit_bytes=60 * 2**20
        ),
        name="reduce",
    )(*terms, part, grad_out)


def on_device(dims, tokens, grad_out, norm_gain, gate_weight, up_weight, down_weight):
    full_tokens, full_grad, gate_full, up_full, down_full = gather_all(
        dims, (tokens, grad_out, gate_weight, up_weight, down_weight)
    )
    floated = full_tokens.astype(jnp.float32)
    inv_rms = lax.rsqrt(jnp.mean(floated * floated, axis=-1, keepdims=True) + 1e-06)
    unit_rows = floated * inv_rms
    gain_rows = norm_gain[None, :]
    normed = (unit_rows * gain_rows).astype(jnp.bfloat16)
    grad_hidden = 0.5 * contract(full_grad, down_full, 1, 1)
    factor = (full_tokens.shape[0] * lax.axis_size("fs")) ** (-0.5)
    gate_pre = contract(normed, gate_full, 1, 1)
    up_pre = contract(normed, up_full, 1, 1)
    sigma = jax.nn.sigmoid(gate_pre)
    active = gate_pre * sigma
    hidden = (active * up_pre).astype(jnp.bfloat16)
    term_down = 0.5 * factor * contract(hidden, full_grad, 0, 0)
    gate_grad_pre = (grad_hidden * up_pre * sigma * (1.0 + gate_pre * (1.0 - sigma))).astype(
        jnp.bfloat16
    )
    term_gate = factor * contract(gate_grad_pre, normed, 0, 0)
    up_grad_pre = (grad_hidden * active).astype(jnp.bfloat16)
    term_up = factor * contract(up_grad_pre, normed, 0, 0)
    grad_rows = jnp.dot(gate_grad_pre, gate_full, preferred_element_type=jnp.float32)
    grad_rows = grad_rows + jnp.dot(up_grad_pre, up_full, preferred_element_type=jnp.float32)
    partial_value = rms_back(grad_rows, unit_rows, inv_rms, gain_rows).astype(jnp.bfloat16)
    terms = [t.astype(jnp.bfloat16) for t in (term_gate, term_up, term_down)]
    grad_gate, grad_up, grad_down, grad_input, row_squares = reduce_all(
        dims, terms, partial_value, grad_out, gate_weight.shape[1]
    )
    return (grad_input, grad_gate, grad_up, grad_down, row_squares)


def solution(mesh):
    in_specs = (P("fs", "tp"), P("fs", "tp"), P(), P("tp", "fs"), P("tp", "fs"), P("tp", "fs"))
    out_specs = (P("fs", "tp"), P("tp", "fs"), P("tp", "fs"), P("tp", "fs"), P(None, "tp"))
    dims = axes_of(mesh.shape["fs"], mesh.shape["tp"])
    return jax.shard_map(
        functools.partial(on_device, dims), mesh=mesh, in_specs=in_specs, out_specs=out_specs,
        check_vma=False,
    )
```
